32 devices in a mesh: ep: 8 (over z, x), tp: 4 (over y, core).
Axes of the slice: x: 2, y: 2, z: 4, core: 2. Of those that a mesh axis runs over, the one named last changes fastest.
Arguments:
- tokens: bfloat16 [2048, 2048], P('ep'), may hold values from -6 to 6
- norm_gain: float32 [2048], replicated, may hold values from 0.1 to 1.9
- expert_ids: int32 [2048, 4], P('ep'), may hold values from 0 to 7, all different within a row; in each aligned block of 256 rows (0 to 255, 256 to 511, ...) at most 256 rows name the same one
- route_weights: float32 [2048, 4], P('ep'), may hold values from 0.05 to 1
- gate_weight: bfloat16 [8, 2048, 2048], P('ep', None, 'tp'), as said below
- up_weight: bfloat16 [8, 2048, 2048], P('ep', None, 'tp'), as said below
- down_weight: bfloat16 [8, 2048, 2048], P('ep', 'tp'), may hold values from -0.125 to 0.125
Outputs:
- mixed: bfloat16 [2048, 2048], P('ep', 'tp')
The draws below stay inside these ranges and needn't reach their ends.
Inputs may be any that keep to these rules, and one draw needn't show every extreme that they name: `expert_ids`: each row names 4 different experts. In the rows of one device no expert is named by more than 256 rows, and in every draw some expert is named by exactly 256 rows of some device. `gate_weight`: independent entries of mean zero, drawn for each expert separately. `up_weight`: independent entries of mean zero, drawn for each expert separately.
All inputs are finite; a program needn't handle non-finite values.
Results may differ from the reference program's by a relative error of at most 0.014.
Values may be sent and summed in bfloat16 or wider, within the bound.
No kernel may reach another device: no remote copies, remote signals or barrier semaphores. Data moves between devices by JAX's collectives and lax.ppermute only.
A program may use at most 128 MiB of HBM per device.

```python
import math
import jax
import jax.numpy as jnp
import numpy as np
from jax import lax

D = 2048
FF = 2048
TOP = 4
TOK_DEV = 256
EXPERTS = 8
CAP = 256
TOKENS = 2048
N_TP = 4


def draw_gate_weight(key, part):
    factor = 1.0
    values = jax.random.normal(jax.random.fold_in(key, 11), (EXPERTS, D, FF), jnp.float32)
    return (values * (factor / D ** 0.5)).astype(jnp.bfloat16)


def draw_up_weight(key, part):
    factor = 1.0
    values = jax.random.normal(jax.random.fold_in(key, 23), (EXPERTS, D, FF), jnp.float32)
    return (values * (factor / D ** 0.5)).astype(jnp.bfloat16)


def levels(stream_key, shape, split, smallest, largest):
    gain, own = 1.0, jax.random.fold_in(stream_key, 6)
    for dim, blocks in split:
        draws = jnp.exp(jax.random.uniform(jax.random.fold_in(own, dim), (blocks,), jnp.float32, smallest / len(split), largest / len(split)))
        gain = gain * jnp.repeat(draws, shape[dim] // blocks).reshape([-1 if axis == dim else 1 for axis in range(len(shape))])
    return gain


def deal_out(own_key, own, number, rows, count, top, most, lean):
    sequence = jax.random.permutation(own_key, count)
    heavy_load, ordinary = portions_of(count, rows * top, most, lean, True), portions_of(count, rows * top, most, lean, False)
    places = jnp.arange(count)

    def named(lengths, rotation):
        used = int((lengths > 0).sum())
        fixed = max(1, used // 4)
        moved = fixed + (places - fixed + rotation * (used - fixed)) % max(1, count - fixed)
        return jnp.zeros((count,), jnp.int32).at[sequence[jnp.where(places < fixed, places, moved)]].set(jnp.asarray(lengths, jnp.int32))

    lengths = jnp.where(number % 4 == 0, named(heavy_load, number // 4), named(ordinary, number - number // 4 - 1))
    mixed = jax.random.permutation(jax.random.fold_in(own, 3), count)
    source_of, sink = mixed[0:count // 2 * 2:2], mixed[1:count // 2 * 2:2]
    slack = jnp.minimum(lengths[source_of] - 1, most - lengths[sink]) // 2
    slack = jnp.where((source_of == sequence[0]) | (sink == sequence[0]) | (lengths[sink] == 0), 0, jnp.maximum(slack, 0))
    moved = jax.random.randint(jax.random.fold_in(own, 4), (count // 2,), 0, 1 << 20) % (slack + 1)
    lengths = lengths.at[source_of].add(-moved).at[sink].add(moved)
    labels = jnp.searchsorted(jnp.cumsum(lengths), jnp.arange(rows * top), side="right").astype(jnp.int32)
    listing = labels.reshape(top, rows).T
    listing = listing[jax.random.permutation(jax.random.fold_in(own, 1), rows)]
    rotation = jax.random.randint(jax.random.fold_in(own, 2), (rows, 1), 0, top)
    return jnp.take_along_axis(listing, (jnp.arange(top)[None, :] + rotation) % top, axis=1)


def portions_of(number_of, total, reach, slope, full):
    portions = [(1 << 20) // math.isqrt(standing ** slope) + 1 for standing in range(1, number_of + 1)]
    largest = reach if full else min(reach, max(-(-total // number_of), total * portions[0] // sum(portions)))
    least = 1 if total - largest >= number_of - 1 else 0
    holding, rest = [largest] + [least] * (number_of - 1), total - largest - least * (number_of - 1)
    while rest > 0:
        movable = [i for i in range(1, number_of) if holding[i] < largest] or [i for i in range(1, number_of) if holding[i] < reach]
        pool, remaining = sum([portions[i] for i in movable]), rest
        for i in movable:
            extra = min(reach - holding[i], max(1, remaining * portions[i] // pool), rest)
            holding[i] = holding[i] + extra
            rest = rest - extra
    return np.array(holding)


def scatter_about(stream_key, dims, scale, reach, shards=(), held_as=jnp.bfloat16):
    values = scale * jax.random.normal(stream_key, dims, jnp.float32)
    if shards:
        values = values * levels(stream_key, dims, shards, -0.22, 0.18)
    return jnp.clip(values, -reach, reach).astype(held_as)


def setup_inputs(seed: int = 0) -> dict:
    key_of = jax.random.split(jax.random.key(seed), 8)
    tokens = scatter_about(key_of[0], (TOKENS, D), 1.0, 6.0, ((0, 8),))
    norm_gain = jnp.clip(1.0 + 0.18 * jax.random.normal(key_of[1], (D,), jnp.float32), 0.1, 1.9)
    expert_ids_keys = jax.random.split(jax.random.fold_in(key_of[2], 1), TOKENS // TOK_DEV)
    expert_ids_turns = jax.random.permutation(jax.random.fold_in(key_of[2], 3), TOKENS // TOK_DEV)
    expert_ids = jax.vmap(lambda own, number: deal_out(jax.random.fold_in(key_of[2], 2), own, number, TOK_DEV, EXPERTS, TOP, CAP, 2))(expert_ids_keys, expert_ids_turns).reshape((TOKENS, TOP))
    route_weights = jnp.clip(0.05 + 0.95 * jax.random.uniform(key_of[3], (TOKENS, TOP), jnp.float32) ** levels(key_of[3], (TOKENS, TOP), ((0, 8),), -0.2, 0.2), 0.05, 1.0)
    gate_weight = draw_gate_weight(jax.random.fold_in(key_of[7], 71), 0)
    up_weight = draw_up_weight(jax.random.fold_in(key_of[7], 71), 0)
    down_weight = scatter_about(key_of[6], (EXPERTS, FF, D), FF ** -0.5, 0.125, ((0, 8), (1, 4)))
    return dict(tokens=tokens, norm_gain=norm_gain, expert_ids=expert_ids, route_weights=route_weights, gate_weight=gate_weight, up_weight=up_weight, down_weight=down_weight)


def reference(tokens, norm_gain, expert_ids, route_weights, gate_weight, up_weight, down_weight):
    values = tokens.astype(jnp.float32)
    scale = lax.rsqrt(lax.optimization_barrier(jnp.mean(values * values, axis=1, keepdims=True)) + 1e-06)
    normed = (values * scale * norm_gain[None, :]).astype(jnp.bfloat16)
    blocks = TOKENS // TOK_DEV
    pairs_dev = TOK_DEV * TOP
    flat = expert_ids.reshape(blocks, pairs_dev)
    onehot = (flat[:, :, None] == jnp.arange(EXPERTS, dtype=jnp.int32)[None, None, :]).astype(jnp.int32)
    before = jnp.cumsum(onehot, axis=1) - onehot
    slot = lax.optimization_barrier(jnp.sum(before * onehot, axis=2))
    source = jnp.arange(blocks, dtype=jnp.int32)[:, None]
    position = (slot + source * CAP).reshape(-1).astype(jnp.int32)
    pair_tok = (source * TOK_DEV + jnp.arange(pairs_dev, dtype=jnp.int32)[None, :] // TOP).reshape(-1).astype(jnp.int32)
    expert_flat = flat.reshape(-1).astype(jnp.int32)
    rows = blocks * CAP
    tok_table = jnp.zeros((EXPERTS, rows), jnp.int32).at[expert_flat, position].set(pair_tok)
    weight_table = jnp.zeros((EXPERTS, rows), jnp.float32).at[expert_flat, position].set(route_weights.reshape(-1))

    def one_expert(total, index):
        chosen = normed[tok_table[index]]
        gate = jnp.dot(chosen, gate_weight[index], preferred_element_type=jnp.float32)
        upper = jnp.dot(chosen, up_weight[index], preferred_element_type=jnp.float32)
        gate = jnp.minimum(gate, 7.0)
        upper = jnp.clip(upper, -7.0, 7.0)
        hidden = ((upper + 1.0) * (gate * jax.nn.sigmoid(1.702 * gate))).astype(jnp.bfloat16)
        blocked = hidden.reshape(rows, N_TP, FF // N_TP).astype(jnp.float32)
        down_blocks = down_weight[index].reshape(N_TP, FF // N_TP, D).astype(jnp.float32)
        partial_value = jnp.einsum('rpf,pfd->rpd', blocked, down_blocks).astype(jnp.bfloat16)
        expert_out = lax.optimization_barrier(jnp.sum(partial_value.astype(jnp.float32), axis=1)).astype(jnp.bfloat16)
        total = total.at[tok_table[index]].add(weight_table[index][:, None] * expert_out.astype(jnp.float32))
        return (total, None)
    start = jnp.zeros((TOKENS, D), jnp.float32)
    total, unused = lax.scan(one_expert, start, jnp.arange(EXPERTS, dtype=jnp.int32))
    return total.astype(jnp.bfloat16)
```

```python
import functools

import jax
import jax.numpy as jnp
from jax import lax
from jax.experimental import pallas as pl
from jax.experimental.pallas import tpu as pltpu
from jax.sharding import PartitionSpec as P


F32 = jnp.float32
BF16 = jnp.bfloat16
LANES = 128
HID_TILE = 256
PIECES = 3


def prep_kernel(core_ref, tokens_ref, gain_ref, ids_ref, weights_ref, out_ref):
    del core_ref
    rows, width = tokens_ref.shape
    experts = out_ref.shape[1] - width
    top = ids_ref.shape[1]
    values = tokens_ref[...].astype(F32)
    scale = lax.rsqrt(jnp.mean(values * values, axis=1, keepdims=True) + 1e-06)
    out_ref[:, :width] = (values * scale * gain_ref[...]).astype(BF16)
    lane = lax.broadcasted_iota(jnp.int32, (rows, experts), 1)
    n_experts = LANES // 4
    dense = jnp.zeros((rows, experts), F32)
    for k in range(top):
        dense = dense + jnp.where((lane % n_experts) == ids_ref[:, k : k + 1], weights_ref[:, k : k + 1], 0.0)
    first = dense.astype(BF16).astype(F32)
    second = (dense - first).astype(BF16).astype(F32)
    third = dense - first - second
    piece = lane // n_experts
    out_ref[:, width:] = jnp.where(piece == 0, first, jnp.where(piece == 1, second, jnp.where(piece == 2, third, 0.0))).astype(BF16)


def prep(core, tokens, gain, ids, weights):
    rows, width = tokens.shape
    half = rows // 2
    top = ids.shape[1]
    return pl.pallas_call(
        prep_kernel,
        out_shape=jax.ShapeDtypeStruct((half, width + LANES), BF16),
        grid_spec=pltpu.PrefetchScalarGridSpec(
            num_scalar_prefetch=1,
            grid=(1,),
            in_specs=[
                pl.BlockSpec((half, width), lambda i, c: (c[0], 0)),
                pl.BlockSpec((1, width), lambda i, c: (0, 0)),
                pl.BlockSpec((half, top), lambda i, c: (c[0], 0)),
                pl.BlockSpec((half, top), lambda i, c: (c[0], 0)),
            ],
            out_specs=pl.BlockSpec((half, width + LANES), lambda i, c: (0, 0)),
        ),
        name="prep",
    )(core, tokens, gain, ids, weights)


def expert_kernel(place_ref, *refs, n_in):
    blocks = refs[:n_in]
    weights = refs[n_in : n_in + 6]
    keep_ref, send_ref = refs[n_in + 6 : n_in + 8]
    x_ref, gate_ref, up_ref, down_ref, acc_ref, x_sem, w_sem = refs[n_in + 8 :]
    rows = blocks[0].shape[0]
    width = x_ref.shape[1] - LANES
    cols = keep_ref.shape[1]
    units = weights[0].shape[1]
    tiles = units // HID_TILE
    copies = []
    for i, block in enumerate(blocks):
        copy = pltpu.make_async_copy(block, x_ref.at[pl.ds(i * rows, rows), :], x_sem.at[i])
        copy.start()
        copies.append(copy)
    plane = place_ref[1]
    fetches = []
    for t in range(2 * tiles):
        gate, up, down = weights[3 * (t // tiles) : 3 * (t // tiles) + 3]
        inner = pl.ds((t % tiles) * HID_TILE, HID_TILE)
        here = pl.ds(t * HID_TILE, HID_TILE)
        mine = pl.ds(pl.multiple_of(plane * cols, LANES), cols)
        theirs = pl.ds(pl.multiple_of((1 - plane) * cols, LANES), cols)
        row = [
            pltpu.make_async_copy(gate.at[:, inner], gate_ref.at[:, here], w_sem.at[4 * t]),
            pltpu.make_async_copy(up.at[:, inner], up_ref.at[:, here], w_sem.at[4 * t + 1]),
            pltpu.make_async_copy(down.at[inner, mine], down_ref.at[here, pl.ds(0, cols)], w_sem.at[4 * t + 2]),
            pltpu.make_async_copy(down.at[inner, theirs], down_ref.at[here, pl.ds(cols, cols)], w_sem.at[4 * t + 3]),
        ]
        for copy in row:
            copy.start()
        fetches.append(row)
    for copy in copies:
        copy.wait()
    lane = lax.broadcasted_iota(jnp.int32, (n_in * rows, LANES), 1)
    own = (lane % (LANES // 4)) == place_ref[0]
    route = jnp.sum(jnp.where(own, x_ref[:, width:].astype(F32), 0.0), axis=1, keepdims=True)
    for t in range(2 * tiles):
        here = pl.ds(t * HID_TILE, HID_TILE)
        for copy in fetches[t]:
            copy.wait()
        gate = jnp.dot(x_ref[:, :width], gate_ref[:, here], preferred_element_type=F32)
        upper = jnp.dot(x_ref[:, :width], up_ref[:, here], preferred_element_type=F32)
        gate = jnp.minimum(gate, 7.0)
        upper = jnp.clip(upper, -7.0, 7.0)
        hidden = (upper + 1.0) * (gate * jax.nn.sigmoid(1.702 * gate))
        hidden = jnp.where(route > 0.0, hidden * route, 0.0).astype(BF16)
        part = jnp.dot(hidden, down_ref[here, :], preferred_element_type=F32)
        if t == 0:
            acc_ref[...] = part
        elif t < 2 * tiles - 1:
            acc_ref[...] += part
        else:
            total = acc_ref[...] + part
            keep_ref[...] = total[:, :cols].astype(BF16)
            send_ref[...] = total[:, cols:].astype(BF16)


def expert(place, blocks, weights):
    rows, wide = blocks[0].shape
    width = wide - LANES
    units = weights[0].shape[1]
    total = len(blocks) * rows
    out = jax.ShapeDtypeStruct((total, width // 2), BF16)
    anywhere = pl.BlockSpec(memory_space=pl.ANY)
    tiles = 2 * units // HID_TILE
    return pl.pallas_call(
        functools.partial(expert_kernel, n_in=len(blocks)),
        out_shape=(out, out),
        in_specs=[pl.BlockSpec(memory_space=pltpu.SMEM)] + [anywhere] * (len(blocks) + 6),
        out_specs=(pl.BlockSpec(memory_space=pltpu.VMEM),) * 2,
        scratch_shapes=[
            pltpu.VMEM((total, wide), BF16),
            pltpu.VMEM((width, 2 * units), BF16),
            pltpu.VMEM((width, 2 * units), BF16),
            pltpu.VMEM((2 * units, width), BF16),
            pltpu.VMEM((total, width), F32),
            pltpu.SemaphoreType.DMA((len(blocks),)),
            pltpu.SemaphoreType.DMA((4 * tiles,)),
        ],
        cost_estimate=pl.CostEstimate(
            flops=2 * total * width * 2 * units * 3,
            bytes_accessed=2 * (6 * width * units + 2 * total * width),
            transcendentals=total * 2 * units,
        ),
        compiler_params=pltpu.CompilerParams(vmem_limit_bytes=40 * 1024 * 1024),
        name="expert",
    )(place, *blocks, *weights)


def routed(tokens, norm_gain, expert_ids, route_weights, gate_weight, up_weight, down_weight):
    tok_dev, width = tokens.shape
    top = expert_ids.shape[1]
    n_ep = lax.axis_size("ep")
    n_tp = lax.axis_size("tp")
    exp_dev = gate_weight.shape[0]
    experts = exp_dev * n_ep
    capacity = 2 * tok_dev * top // experts
    quarter = width // n_tp
    values = tokens.astype(jnp.float32)
    scale = lax.rsqrt(jnp.mean(values * values, axis=1, keepdims=True) + 1e-06)
    normed = (values * scale * norm_gain[None, :]).astype(jnp.bfloat16)
    flat = expert_ids.reshape(-1)
    count = flat.shape[0]
    onehot = (flat[:, None] == jnp.arange(experts, dtype=jnp.int32)[None, :]).astype(jnp.int32)
    before = jnp.cumsum(onehot, axis=0) - onehot
    slot = jnp.sum(before * onehot, axis=1)
    position = flat * capacity + slot
    source_tok = jnp.arange(count, dtype=jnp.int32) // top
    buffer_tok = jnp.zeros((experts * capacity,), jnp.int32).at[position].set(source_tok)
    buffer_live = jnp.zeros((experts * capacity,), jnp.int32).at[position].set(1)
    columns = lax.dynamic_slice_in_dim(normed, lax.axis_index("tp") * quarter, quarter, 1)
    outgoing = jnp.where(buffer_live[:, None] > 0, columns[buffer_tok], jnp.zeros((), jnp.bfloat16))
    outgoing = outgoing.reshape(n_ep, exp_dev, capacity, quarter)
    received = lax.all_gather(
        lax.all_to_all(outgoing, "ep", split_axis=0, concat_axis=0, tiled=True),
        "tp",
        axis=3,
        tiled=True,
    )
    gate = jnp.einsum("sxcd,xdf->sxcf", received, gate_weight, preferred_element_type=jnp.float32)
    upper = jnp.einsum("sxcd,xdf->sxcf", received, up_weight, preferred_element_type=jnp.float32)
    gate = jnp.minimum(gate, 7.0)
    upper = jnp.clip(upper, -7.0, 7.0)
    hidden = ((upper + 1.0) * (gate * jax.nn.sigmoid(1.702 * gate))).astype(jnp.bfloat16)
    partial_value = jnp.einsum(
        "sxcf,xfd->sxcd", hidden, down_weight, preferred_element_type=jnp.float32
    )
    rounded = partial_value.astype(jnp.bfloat16)
    summed = (
        lax.psum_scatter(rounded, "tp", scatter_dimension=3, tiled=True)
        .astype(jnp.float32)
        .astype(jnp.bfloat16)
    )
    returned = lax.all_to_all(summed, "ep", split_axis=0, concat_axis=0, tiled=True)
    returned = returned.reshape(experts * capacity, quarter)
    picked = returned[position].reshape(tok_dev, top, quarter)
    mixed = jnp.sum(route_weights[:, :, None] * picked.astype(jnp.float32), axis=1)
    return mixed.astype(jnp.bfloat16)


def dense(tokens, norm_gain, expert_ids, route_weights, gate_weight, up_weight, down_weight):
    n_ep = lax.axis_size("ep")
    n_tp = lax.axis_size("tp")
    tok_dev, width = tokens.shape
    quarter = width // n_tp
    half = tok_dev // 2
    part = lax.axis_index("tp")
    core, plane = part % 2, part // 2

    def permute(value, ep_mask, tp_mask):
        pairs = [
            (e * n_tp + t, (e ^ ep_mask) * n_tp + (t ^ tp_mask)) for e in range(n_ep) for t in range(n_tp)
        ]
        return lax.ppermute(value, ("ep", "tp"), pairs)

    own = (gate_weight[0], up_weight[0], down_weight[0])
    block = prep(core.reshape(1), tokens, norm_gain.reshape(1, width), expert_ids, route_weights)
    steps = n_ep // 2
    pairs = [[block, permute(block, 1, 0)]]
    far = [permute(block, 2 * k, 0) for k in range(1, steps)]
    other = tuple(permute(value, 0, 1) for value in own)
    for value in far:
        pairs.append([value, permute(value, 1, 0)])
    place = jnp.stack([lax.axis_index("ep"), plane]).astype(jnp.int32)
    parts = []
    for k in range(steps):
        keep, send = expert(place, pairs[k], own + other)
        got = permute(send, 0, 2)
        mine = keep.astype(F32) + got.astype(F32)
        across = permute(mine[half:].astype(BF16), 1, 0)
        mine = mine[:half] + across.astype(F32)
        if k:
            mine = permute(mine.astype(BF16), 2 * k, 0).astype(F32)
        parts.append(mine)
    total = functools.reduce(lambda a, b: a + b, parts).astype(BF16)
    mine = lax.dynamic_slice_in_dim(total, core * quarter, quarter, 1)
    given = permute(lax.dynamic_slice_in_dim(total, (1 - core) * quarter, quarter, 1), 0, 1)
    return jnp.where(core == 0, jnp.concatenate([mine, given]), jnp.concatenate([given, mine]))


def per_device(tokens, norm_gain, expert_ids, route_weights, gate_weight, up_weight, down_weight):
    n_ep = lax.axis_size("ep")
    n_tp = lax.axis_size("tp")
    tok_dev, top = expert_ids.shape
    width = tokens.shape[1]
    exp_dev, _, units = gate_weight.shape
    experts = exp_dev * n_ep
    everyone = 2 * tok_dev * top // experts >= tok_dev
    fits = exp_dev == 1 and n_tp == 4 and n_ep & (n_ep - 1) == 0 and n_ep > 1 and experts <= LANES // 4
    tiled = tok_dev % 32 == 0 and width % (2 * n_tp * LANES) == 0 and units % HID_TILE == 0
    run = dense if everyone and fits and tiled else routed
    return run(tokens, norm_gain, expert_ids, route_weights, gate_weight, up_weight, down_weight)


def solution(mesh):
    in_specs = (
        P("ep", None),
        P(),
        P("ep", None),
        P("ep", None),
        P("ep", None, "tp"),
        P("ep", None, "tp"),
        P("ep", "tp", None),
    )
    out_specs = P("ep", "tp")
    return jax.shard_map(
        per_device, mesh=mesh, in_specs=in_specs, out_specs=out_specs, check_vma=False
    )
```
